32 devices in a mesh: sp: 4 (over z), fs: 4 (over y, x), tp: 2 (over core).
Axes of the slice: x: 2, y: 2, z: 4, core: 2. Of those that a mesh axis runs over, the one named last changes fastest.
Arguments:
- tokens: bfloat16 [4, 8192, 2048], P('fs', 'sp'), may hold values from -21 to 21
- norm_gain: float32 [2048], replicated, may hold values from 0.1 to 1.9
- w_query: bfloat16 [2048, 1024], P(None, 'tp'), may hold values from -0.125 to 0.125
- w_key: bfloat16 [2048, 256], P(None, 'tp'), may hold values from -0.125 to 0.125
- w_value: bfloat16 [2048, 256], P(None, 'tp'), may hold values from -0.125 to 0.125
- w_pool: bfloat16 [2048, 1024], P(None, 'tp'), may hold values from -0.125 to 0.125
- w_group: bfloat16 [4, 256, 256], P('tp'), may hold values from -0.375 to 0.375
- w_out: bfloat16 [2048, 2048], replicated, may hold values from -0.125 to 0.125
- sinks: float32 [16], P('tp'), may hold values from -1 to 260
Outputs:
- mixed: bfloat16 [4, 8192, 2048], P('fs', ('sp', 'tp'))
- log_sums: float32 [4, 16, 8192], P('fs', 'tp', 'sp')
The draws below stay inside these ranges and needn't reach their ends.
All inputs are finite; a program needn't handle non-finite values.
Results may differ from the reference program's by a relative error of at most 0.009.
Values may be sent and summed in bfloat16 or wider, within the bound.
No kernel may reach another device: no remote copies, remote signals or barrier semaphores. Data moves between devices by JAX's collectives and lax.ppermute only.
A program may use at most 192 MiB of HBM per device.

```python
import jax
import jax.numpy as jnp
from jax import lax

D = 2048
HEAD_SIZE = 64
QUERY_HEADS = 16
KEY_VALUE_HEADS = 4
GROUPS = 4
GDIM = 256
WINDOW_KEYS = 128
SEQS = 4
LEN = 8192
PW = 1024
QW = 1024
KW = 256


def draw_tokens(key, part):
    subkeys = jax.random.split(jax.random.fold_in(key, 11), 5)
    noise_part = jnp.clip(jax.random.normal(subkeys[0], (SEQS, LEN, D), jnp.float32), -4.0, 4.0)
    drift_sign = jnp.where(jax.random.uniform(subkeys[3], (SEQS, 1, 1), jnp.float32) < 0.5, -1.0, 1.0)
    drift_level = drift_sign * jax.random.uniform(subkeys[2], (SEQS, 1, 1), jnp.float32, 0.4, 1.0)
    rough_part = jax.random.uniform(subkeys[4], (SEQS, LEN // 32, 1), jnp.float32, -0.8, 0.8)
    direction = jnp.clip(jax.random.normal(subkeys[1], (SEQS, 1, D), jnp.float32), -3.0, 3.0)
    rise_factor = 1.0 + 2.0 * jnp.arange(LEN, dtype=jnp.float32)[None, :, None] / LEN
    amplitude = drift_level * rise_factor + jnp.repeat(rough_part, 32, axis=1)
    return (noise_part + amplitude * direction).astype(jnp.bfloat16)


def draw_sinks(key, part):
    subkeys = jax.random.split(jax.random.fold_in(key, 23), 1)
    sink_values = jax.random.uniform(subkeys[0], (QUERY_HEADS,), jnp.float32, -1.0, 6.0)
    return sink_values


def shard_levels(key, shape, pieces, smallest, high):
    factor_of, own = 1.0, jax.random.fold_in(key, 6)
    for position, shards_of in pieces:
        draws = jnp.exp(jax.random.uniform(jax.random.fold_in(own, position), (shards_of,), jnp.float32, smallest / len(pieces), high / len(pieces)))
        factor_of = factor_of * jnp.repeat(draws, shape[position] // shards_of).reshape([-1 if axis == position else 1 for axis in range(len(shape))])
    return factor_of


def scatter_about(stream_key, dims, width, bound, cuts=(), kind=jnp.bfloat16):
    entries = jax.random.normal(stream_key, dims, jnp.float32) * width
    if len(cuts) > 0:
        entries = shard_levels(stream_key, dims, cuts, -0.22, 0.18) * entries
    return jnp.clip(entries, min=-bound, max=bound).astype(kind)


def setup_inputs(seed: int = 0) -> dict:
    streams_of = jax.random.split(jax.random.key(seed), 10)
    return {
        "tokens": draw_tokens(jax.random.fold_in(streams_of[9], 71), 0),
        "norm_gain": jnp.clip(1.0 + 0.18 * jax.random.normal(streams_of[1], (D,), jnp.float32), 0.1, 1.9),
        "w_query": scatter_about(streams_of[2], (D, QW), D ** -0.5, 0.125, ((1, 2),)),
        "w_key": scatter_about(streams_of[3], (D, KW), D ** -0.5, 0.125, ((1, 2),)),
        "w_value": scatter_about(streams_of[4], (D, KW), D ** -0.5, 0.125, ((1, 2),)),
        "w_pool": scatter_about(streams_of[5], (D, PW), D ** -0.5, 0.125, ((1, 2),)),
        "w_group": scatter_about(streams_of[6], (GROUPS, GDIM, GDIM), GDIM ** -0.5, 0.375, ((0, 2),)),
        "w_out": scatter_about(streams_of[7], (PW + QW, D), (PW + QW) ** -0.5, 0.125),
        "sinks": draw_sinks(jax.random.fold_in(streams_of[9], 71), 0),
    }


LN_EPS = 1e-05

def normalize(token_rows, norm_gain):
    values = token_rows.astype(jnp.float32)
    row_mean = lax.optimization_barrier(jnp.mean(values, axis=-1, keepdims=True))
    centered = values - row_mean
    variance = lax.optimization_barrier(jnp.mean(centered * centered, axis=-1, keepdims=True))
    return (centered * lax.rsqrt(variance + LN_EPS) * norm_gain).astype(jnp.bfloat16)

def pool_branch(pool_rows, w_group):
    length = pool_rows.shape[0]
    reach = 2 ** GROUPS - 1
    values = pool_rows.astype(jnp.float32)
    padded = jnp.pad(values, ((reach, 0), (0, 0)))
    positions = jnp.arange(length, dtype=jnp.int32)
    prefix_mean = jnp.cumsum(values, axis=0) / (positions + 1).astype(jnp.float32)[:, None]
    outputs = []
    for group_index in range(GROUPS):
        span_width = 2 ** (group_index + 1)
        first_col = group_index * GDIM
        window_sum = jnp.zeros((length, GDIM), jnp.float32)
        for offset in range(span_width):
            window_sum = window_sum + padded[reach - offset:reach - offset + length, first_col:first_col + GDIM]
        window_count = jnp.minimum(positions + 1, span_width).astype(jnp.float32)[:, None]
        pooled = (window_sum / window_count - prefix_mean[:, first_col:first_col + GDIM]).astype(jnp.bfloat16)
        outputs.append(jnp.dot(pooled, w_group[group_index], preferred_element_type=jnp.float32).astype(jnp.bfloat16))
    return jnp.concatenate(outputs, axis=1)

def attention_branch(query_matrix, key_rows, value_rows, sinks):
    length = query_matrix.shape[0]
    block_extent = min(512, length)
    heads_per_group = QUERY_HEADS // KEY_VALUE_HEADS
    padded_keys = jnp.pad(key_rows, ((WINDOW_KEYS, 0), (0, 0)))
    padded_values = jnp.pad(value_rows, ((WINDOW_KEYS, 0), (0, 0)))
    attention_sink_logits = sinks.astype(jnp.float32).reshape(KEY_VALUE_HEADS, heads_per_group)[:, :, None, None]

    def one_block(block_index):
        start_row = (block_index * block_extent).astype(jnp.int32)
        query_tile_rows = lax.dynamic_slice_in_dim(query_matrix, start_row, block_extent, 0).reshape(block_extent, KEY_VALUE_HEADS, heads_per_group, HEAD_SIZE)
        key_tile_rows = lax.dynamic_slice_in_dim(padded_keys, start_row, block_extent + WINDOW_KEYS, 0).reshape(block_extent + WINDOW_KEYS, KEY_VALUE_HEADS, HEAD_SIZE)
        value_tile_rows = lax.dynamic_slice_in_dim(padded_values, start_row, block_extent + WINDOW_KEYS, 0).reshape(block_extent + WINDOW_KEYS, KEY_VALUE_HEADS, HEAD_SIZE)
        scores = jnp.einsum('qhrd,khd->hrqk', query_tile_rows.astype(jnp.float32), key_tile_rows.astype(jnp.float32)) * HEAD_SIZE ** (-0.5)
        query_positions = start_row + jnp.arange(block_extent, dtype=jnp.int32)
        key_positions = start_row - WINDOW_KEYS + jnp.arange(block_extent + WINDOW_KEYS, dtype=jnp.int32)
        distance = query_positions[:, None] - key_positions[None, :]
        visible = (distance >= 0) & (distance < WINDOW_KEYS) & (key_positions >= 0)[None, :]
        scores = jnp.where(visible, scores, -jnp.inf)
        row_max = jnp.maximum(lax.optimization_barrier(jnp.max(scores, axis=-1, keepdims=True)), attention_sink_logits)
        weights = jnp.exp(scores - row_max)
        weight_sum = lax.optimization_barrier(jnp.sum(weights, axis=-1, keepdims=True)) + jnp.exp(attention_sink_logits - row_max)
        normalized = (weights / weight_sum).astype(jnp.bfloat16)
        block_out = jnp.einsum('hrqk,khd->qhrd', normalized.astype(jnp.float32), value_tile_rows.astype(jnp.float32))
        block_out = block_out.astype(jnp.bfloat16).reshape(block_extent, QUERY_HEADS * HEAD_SIZE)
        block_logs = (row_max + jnp.log(weight_sum))[..., 0].reshape(QUERY_HEADS, block_extent)
        return (block_out, block_logs)
    block_outs, block_logs = lax.map(one_block, jnp.arange(length // block_extent, dtype=jnp.int32))
    attn_out = block_outs.reshape(length, QUERY_HEADS * HEAD_SIZE)
    log_sums = jnp.transpose(block_logs, (1, 0, 2)).reshape(QUERY_HEADS, length)
    return (attn_out, log_sums)

def reference(tokens, norm_gain, w_query, w_key, w_value, w_pool, w_group, w_out, sinks):

    def one_sequence(token_rows):
        normed = normalize(token_rows, norm_gain)
        query_matrix = jnp.dot(normed, w_query, preferred_element_type=jnp.float32).astype(jnp.bfloat16)
        key_rows = jnp.dot(normed, w_key, preferred_element_type=jnp.float32).astype(jnp.bfloat16)
        value_rows = jnp.dot(normed, w_value, preferred_element_type=jnp.float32).astype(jnp.bfloat16)
        pool_rows = jnp.dot(normed, w_pool, preferred_element_type=jnp.float32).astype(jnp.bfloat16)
        pool_out = pool_branch(pool_rows, w_group)
        attn_out, log_sums = attention_branch(query_matrix, key_rows, value_rows, sinks)
        joined = jnp.concatenate([pool_out, attn_out], axis=1)
        mixed = jnp.dot(joined, w_out, preferred_element_type=jnp.float32).astype(jnp.bfloat16)
        return (mixed, log_sums)
    mixed, log_sums = lax.map(one_sequence, tokens)
    return (mixed, log_sums)
```

```python
import jax
import jax.numpy as jnp
from jax import lax
from jax.experimental import pallas as pl
from jax.experimental.pallas import tpu as pltpu
from jax.sharding import PartitionSpec as P

HEAD_SIZE = 64
GROUPS = 4
GDIM = 256
WINDOW_KEYS = 128
LN_EPS = 1e-05

ROWS = 512
TILE = 256
REACH = 16
F32 = jnp.float32
BF16 = jnp.bfloat16


def dot(a, b, dims=((1,), (0,))):
    return lax.dot_general(a, b, (dims, ((), ())), preferred_element_type=F32)


def project_kernel(x_ref, gain_ref, wk_ref, wv_ref, wp_ref, n_ref, kv_ref, p_ref, sums_ref,
                   tail_ref, tot_ref, wkv, total):
    step = pl.program_id(0)
    last = pl.num_programs(0) - 1
    kw = wk_ref.shape[1]
    pw = wp_ref.shape[1]

    @pl.when(step == 0)
    def _():
        wkv[:, :kw] = wk_ref[...]
        wkv[:, kw:] = wv_ref[...]
        total[...] = jnp.zeros_like(total)

    rows = x_ref.shape[0]
    gain = gain_ref[...]
    running = total[0:1]
    for part in range(rows // TILE):
        span = slice(part * TILE, (part + 1) * TILE)
        x = x_ref[span].astype(F32)
        centered = x - jnp.mean(x, axis=-1, keepdims=True)
        variance = jnp.mean(centered * centered, axis=-1, keepdims=True)
        normed = (centered * lax.rsqrt(variance + LN_EPS) * gain).astype(BF16)
        n_ref[span] = normed
        kv_ref[span] = dot(normed, wkv[...]).astype(BF16)
        pool = dot(normed, wp_ref[...]).astype(BF16)
        p_ref[span] = pool
        part_sum = jnp.sum(pool.astype(F32), axis=0, keepdims=True)
        sums_ref[pl.ds(step * (rows // TILE) + part, 1)] = part_sum
        running = running + part_sum
    total[0:1] = running

    @pl.when(step == last)
    def _():
        hi = running.astype(BF16).astype(F32)
        mid = (running - hi).astype(BF16).astype(F32)
        low = running - hi - mid
        tot = jnp.concatenate([hi, mid, low, jnp.zeros((REACH - 3, pw), F32)], axis=0).astype(BF16)
        tot_ref[...] = tot
        tail_ref[...] = jnp.zeros_like(tail_ref)
        tail_ref[:WINDOW_KEYS, : 2 * kw] = kv_ref[rows - WINDOW_KEYS :]
        tail_ref[WINDOW_KEYS : WINDOW_KEYS + REACH] = p_ref[rows - REACH :]
        tail_ref[WINDOW_KEYS + REACH :] = tot


def project(x, gain, wk, wv, wp):
    length, d = x.shape
    kw, pw = wk.shape[1], wp.shape[1]
    rows = min(ROWS, length)
    whole = lambda shape: pl.BlockSpec(shape, lambda i: (0, 0))
    tail_rows = WINDOW_KEYS + 2 * REACH
    return pl.pallas_call(
        project_kernel,
        name="project",
        grid=(length // rows,),
        in_specs=[
            pl.BlockSpec((rows, d), lambda i: (i, 0)),
            whole((1, d)),
            whole((d, kw)),
            whole((d, kw)),
            whole((d, pw)),
        ],
        out_specs=[
            pl.BlockSpec((rows, d), lambda i: (i, 0)),
            pl.BlockSpec((rows, 2 * kw), lambda i: (i, 0)),
            pl.BlockSpec((rows, pw), lambda i: (i, 0)),
            whole((length // TILE, pw)),
            whole((tail_rows, pw)),
            whole((REACH, pw)),
        ],
        out_shape=[
            jax.ShapeDtypeStruct((length, d), BF16),
            jax.ShapeDtypeStruct((length, 2 * kw), BF16),
            jax.ShapeDtypeStruct((length, pw), BF16),
            jax.ShapeDtypeStruct((length // TILE, pw), F32),
            jax.ShapeDtypeStruct((tail_rows, pw), BF16),
            jax.ShapeDtypeStruct((REACH, pw), BF16),
        ],
        scratch_shapes=[pltpu.VMEM((d, 2 * kw), BF16), pltpu.VMEM((8, pw), F32)],
        cost_estimate=pl.CostEstimate(
            flops=2 * length * d * (2 * kw + pw), bytes_accessed=6 * length * d, transcendentals=0
        ),
        compiler_params=pltpu.CompilerParams(dimension_semantics=("arbitrary",)),
    )(x, gain, wk, wv, wp)


def query_kernel(n_ref, w_ref, q_ref):
    q_ref[...] = (dot(n_ref[...], w_ref[...]) * HEAD_SIZE ** (-0.5)).astype(BF16)


def project_queries(normed, wq):
    length, d = normed.shape
    qw = wq.shape[1]
    rows = min(ROWS, length)
    return pl.pallas_call(
        query_kernel,
        name="queries",
        grid=(length // rows,),
        in_specs=[
            pl.BlockSpec((rows, d), lambda i: (i, 0)),
            pl.BlockSpec((d, qw), lambda i: (0, 0)),
        ],
        out_specs=pl.BlockSpec((rows, qw), lambda i: (i, 0)),
        out_shape=jax.ShapeDtypeStruct((length, qw), BF16),
        cost_estimate=pl.CostEstimate(
            flops=2 * length * d * qw, bytes_accessed=2 * length * d, transcendentals=0
        ),
        compiler_params=pltpu.CompilerParams(dimension_semantics=("arbitrary",)),
    )(normed, wq)


def mixer_kernel(further, where_ref, q_ref, kv_ref, kvp_ref, p_ref, pp_ref, sums_ref, tail_ref,
                 *refs):
    tots = refs[:further]
    wg_ref, sink_ref, _, act_ref, log_ref = refs[further:]
    seq_part = where_ref[1]
    tile = where_ref[0] * pl.num_programs(0) + pl.program_id(0)
    first = tile == 0
    rows, qw = q_ref.shape
    kw = kv_ref.shape[1] // 2
    pw = p_ref.shape[1]
    length = sums_ref.shape[0] * rows

    x = p_ref[...]
    row = lax.broadcasted_iota(jnp.int32, (rows, rows), 0)
    col = lax.broadcasted_iota(jnp.int32, (rows, rows), 1)
    gap = row - col
    lower = jnp.where(gap >= 0, 1.0, 0.0).astype(BF16)
    before = lax.broadcasted_iota(jnp.int32, sums_ref.shape, 0) < tile
    carry = jnp.sum(jnp.where(before, sums_ref[...], 0.0), axis=0, keepdims=True)
    for got in (tail_ref[WINDOW_KEYS + REACH :],) + tuple(t[...] for t in tots):
        carry = carry + jnp.sum(got.astype(F32), axis=0, keepdims=True)
    prev_pool = jnp.where(
        first, tail_ref[WINDOW_KEYS : WINDOW_KEYS + REACH].astype(F32), pp_ref[...].astype(F32)
    ).astype(BF16)
    spot = seq_part * length + tile * rows + lax.broadcasted_iota(jnp.int32, (rows, 1), 0) + 1
    inverse_spot = 1.0 / spot.astype(F32)
    edge_gap = (
        lax.broadcasted_iota(jnp.int32, (REACH, REACH), 0)
        + REACH
        - lax.broadcasted_iota(jnp.int32, (REACH, REACH), 1)
    )
    for slot in range(pw // GDIM):
        lanes = slice(slot * GDIM, (slot + 1) * GDIM)
        width = jnp.left_shift(jnp.int32(2), where_ref[2] * (pw // GDIM) + slot)
        band = jnp.where((gap >= 0) & (gap < width), 1.0, 0.0).astype(BF16)
        edge = jnp.where(edge_gap < width, 1.0, 0.0).astype(BF16)
        window = dot(band, x[:, lanes])
        window = jnp.concatenate(
            [window[:REACH] + dot(edge, prev_pool[:, lanes]), window[REACH:]], axis=0
        )
        prefix = dot(lower, x[:, lanes]) + carry[:, lanes]
        inverse_count = 1.0 / jnp.minimum(spot, width).astype(F32)
        pooled = (window * inverse_count - prefix * inverse_spot).astype(BF16)
        act_ref[:, lanes] = dot(pooled, wg_ref[slot]).astype(BF16)

    wk = WINDOW_KEYS
    key = lax.broadcasted_iota(jnp.int32, (wk, wk), 0)
    query = lax.broadcasted_iota(jnp.int32, (wk, wk), 1)
    is_prev = key > query
    prev_one = jnp.where(is_prev, 1.0, 0.0).astype(BF16)
    own_one = jnp.where(is_prev, 0.0, 1.0).astype(BF16)
    kv_prev = jnp.where(
        first, tail_ref[:wk, : 2 * kw].astype(F32), kvp_ref[...].astype(F32)
    ).astype(BF16)
    no_prev = jnp.where(first & (seq_part == 0), -1e30, 0.0).astype(F32)
    kv_count = kw // HEAD_SIZE
    pairs = qw // HEAD_SIZE // kv_count // 2
    two = 2 * HEAD_SIZE
    for block in range(rows // wk):
        span = slice(block * wk, (block + 1) * wk)
        own = kv_ref[span]
        both = jnp.concatenate([kv_prev, own], axis=0)
        keys = both[:, :kw]
        values_t = both[:, kw:].astype(F32).T.astype(BF16)
        for kv_head in range(kv_count):
            head_key = keys[:, kv_head * HEAD_SIZE : (kv_head + 1) * HEAD_SIZE]
            blank = jnp.zeros_like(head_key)
            stacked = jnp.concatenate(
                [
                    jnp.concatenate([head_key, blank], axis=1),
                    jnp.concatenate([blank, head_key], axis=1),
                ],
                axis=0,
            )
            base = kv_head * pairs
            queries = jnp.concatenate(
                [q_ref[span, (base + p) * two : (base + p + 1) * two] for p in range(pairs)], axis=0
            )
            scores = dot(stacked, queries, ((1,), (1,)))
            head_values = values_t[kv_head * HEAD_SIZE : (kv_head + 1) * HEAD_SIZE]
            halves = []
            for odd in range(2):
                columns = []
                scales = []
                for p in range(pairs):
                    head = (base + p) * 2 + odd
                    cols = slice(p * wk, (p + 1) * wk)
                    seen = jnp.where(
                        is_prev,
                        scores[odd * 2 * wk : odd * 2 * wk + wk, cols] + no_prev
                        if block == 0
                        else scores[odd * 2 * wk : odd * 2 * wk + wk, cols],
                        scores[odd * 2 * wk + wk : (odd + 1) * 2 * wk, cols],
                    )
                    sink = sink_ref[head]
                    row_max = jnp.maximum(jnp.max(seen, axis=0, keepdims=True), sink)
                    weights = jnp.exp(seen - row_max)
                    weight_sum = jnp.sum(weights, axis=0, keepdims=True) + jnp.exp(sink - row_max)
                    log_ref[head : head + 1, span] = row_max + jnp.log(weight_sum)
                    weights = weights.astype(BF16)
                    columns.append(
                        jnp.concatenate([weights * prev_one, weights * own_one], axis=0)
                    )
                    scales.append(1.0 / weight_sum)
                out = dot(head_values, jnp.concatenate(columns, axis=1))
                halves.append(out * jnp.concatenate(scales, axis=1))
            for p in range(pairs):
                cols = slice(p * wk, (p + 1) * wk)
                pair = jnp.concatenate([halves[0][:, cols], halves[1][:, cols]], axis=0).T
                first_lane = pw + (base + p) * two
                act_ref[span, first_lane : first_lane + two] = pair.astype(BF16)
        kv_prev = own


def mix(where, q, kv, pool, sums, tail, tots, w_group, sinks, logs, steps):
    length, qw = q.shape
    kw2, pw = kv.shape[1], pool.shape[1]
    tile = lambda i, w: w[0] * steps + i
    spec = pl.BlockSpec
    heads = qw // HEAD_SIZE
    in_specs = [
        spec((TILE, qw), lambda i, w: (tile(i, w), 0)),
        spec((TILE, kw2), lambda i, w: (tile(i, w), 0)),
        spec((WINDOW_KEYS, kw2), lambda i, w: (jnp.maximum(tile(i, w) * (TILE // WINDOW_KEYS) - 1, 0), 0)),
        spec((TILE, pw), lambda i, w: (tile(i, w), 0)),
        spec((REACH, pw), lambda i, w: (jnp.maximum(tile(i, w) * (TILE // REACH) - 1, 0), 0)),
        spec(sums.shape, lambda i, w: (0, 0)),
        spec(tail.shape, lambda i, w: (0, 0)),
    ]
    in_specs += [spec(t.shape, lambda i, w: (0, 0)) for t in tots]
    in_specs += [
        spec(w_group.shape, lambda i, w: (0, 0, 0)),
        spec(memory_space=pltpu.SMEM),
        spec(memory_space=pl.ANY),
    ]
    operands = (where, q, kv, kv, pool, pool, sums, tail, *tots, w_group, sinks, logs)
    return pl.pallas_call(
        lambda *refs: mixer_kernel(len(tots), *refs),
        name="mixer",
        grid_spec=pltpu.PrefetchScalarGridSpec(
            num_scalar_prefetch=1,
            grid=(steps,),
            in_specs=in_specs,
            out_specs=[
                spec((TILE, pw + qw), lambda i, w: (i, 0)),
                spec((heads, TILE), lambda i, w: (0, tile(i, w))),
            ],
        ),
        out_shape=[
            jax.ShapeDtypeStruct((steps * TILE, pw + qw), BF16),
            jax.ShapeDtypeStruct((heads, length), F32),
        ],
        input_output_aliases={len(operands) - 1: 1},
        cost_estimate=pl.CostEstimate(
            flops=8 * steps * TILE * (WINDOW_KEYS * qw + TILE * pw),
            bytes_accessed=6 * steps * TILE * (pw + qw),
            transcendentals=0,
        ),
        compiler_params=pltpu.CompilerParams(dimension_semantics=("arbitrary",)),
    )(*operands)


def output_kernel(where_ref, a_ref, b_ref, wa0, wa1, wb0, wb1, o_ref):
    half = wa0.shape[1]
    total = dot(a_ref[:, :half], wa0[0]) + dot(a_ref[:, half:], wa1[0])
    total = total + dot(b_ref[:, :half], wb0[0]) + dot(b_ref[:, half:], wb1[0])
    o_ref[...] = total.astype(BF16)


def project_out(where, own, other, w_out, width):
    rows, inner = own.shape
    d = w_out.shape[1]
    chunk = inner // 2
    blocks = w_out.reshape(w_out.shape[0] // chunk, chunk, d)
    spec = pl.BlockSpec
    weight = lambda place: spec((1, chunk, width), lambda j, w: (place(w[2]), 0, j))
    return pl.pallas_call(
        output_kernel,
        name="output",
        grid_spec=pltpu.PrefetchScalarGridSpec(
            num_scalar_prefetch=1,
            grid=(d // width,),
            in_specs=[
                spec((rows, inner), lambda j, w: (0, 0)),
                spec((rows, inner), lambda j, w: (0, 0)),
                weight(lambda t: t),
                weight(lambda t: 2 + t),
                weight(lambda t: 1 - t),
                weight(lambda t: 3 - t),
            ],
            out_specs=spec((rows, width), lambda j, w: (0, j)),
        ),
        out_shape=jax.ShapeDtypeStruct((rows, d), BF16),
        cost_estimate=pl.CostEstimate(
            flops=4 * rows * inner * d, bytes_accessed=6 * rows * d, transcendentals=0
        ),
        compiler_params=pltpu.CompilerParams(dimension_semantics=("arbitrary",)),
    )(where, own, other, blocks, blocks, blocks, blocks)


def body(tokens, norm_gain, w_query, w_key, w_value, w_pool, w_group, w_out, sinks):
    x = tokens[0]
    length = x.shape[0]
    parts = lax.axis_size("sp")
    sp, tp = lax.axis_index("sp"), lax.axis_index("tp")
    normed, kv, pool, sums, tail, tot = project(x, norm_gain[None, :], w_key, w_value, w_pool)
    ahead = lambda value, steps: lax.ppermute(
        value, "sp", [(source, source + steps) for source in range(parts - steps)]
    )
    tail = ahead(tail, 1)
    tots = [ahead(tot, steps) for steps in range(2, parts)]
    q = project_queries(normed, w_query)
    steps = length // TILE // 2
    heads = q.shape[1] // HEAD_SIZE
    place = lambda half: jnp.stack([half, sp, tp]).astype(jnp.int32)
    logs = jnp.zeros((heads, length), F32)
    sent, logs = mix(place(1 - tp), q, kv, pool, sums, tail, tots, w_group, sinks, logs, steps)
    other = lax.ppermute(sent, "tp", [(0, 1), (1, 0)])
    own, logs = mix(place(tp), q, kv, pool, sums, tail, tots, w_group, sinks, logs, steps)
    mixed = project_out(place(tp), own, other, w_out, 512)
    return (mixed[None], logs[None])


def solution(mesh):
    return jax.shard_map(
        body,
        mesh=mesh,
        in_specs=(
            P("fs", "sp", None),
            P(),
            P(None, "tp"),
            P(None, "tp"),
            P(None, "tp"),
            P(None, "tp"),
            P("tp", None, None),
            P(),
            P("tp"),
        ),
        out_specs=(P("fs", ("sp", "tp"), None), P("fs", "tp", "sp")),
        check_vma=False,
    )
```

```python
import jax
import jax.numpy as jnp
from jax import lax
from jax.experimental import pallas as pl
from jax.experimental.pallas import tpu as pltpu
from jax.sharding import PartitionSpec as P

HEAD_SIZE = 64
GROUPS = 4
GDIM = 256
WINDOW_KEYS = 128
LN_EPS = 1e-05

ROWS = 512
TILE = 256
PIECE = 16
REACH = 16
F32 = jnp.float32
BF16 = jnp.bfloat16


def dot(a, b, dims=((1,), (0,))):
    return lax.dot_general(a, b, (dims, ((), ())), preferred_element_type=F32)


def project_kernel(x_ref, gain_ref, wq_ref, wk_ref, wv_ref, wp_ref, q_ref, kv_ref, p_ref, sums_ref,
                   tail_ref, tot_ref, wkv, total, n_ref):
    step = pl.program_id(0)
    last = pl.num_programs(0) - 1
    kw = wk_ref.shape[1]
    pw = wp_ref.shape[1]

    @pl.when(step == 0)
    def _():
        wkv[:, :kw] = wk_ref[...]
        wkv[:, kw:] = wv_ref[...]
        total[...] = jnp.zeros_like(total)

    rows = x_ref.shape[0]
    gain = gain_ref[...]
    running = total[0:1]
    for part in range(rows // TILE):
        span = slice(part * TILE, (part + 1) * TILE)
        for piece in range(TILE // PIECE):
            lines = slice(part * TILE + piece * PIECE, part * TILE + (piece + 1) * PIECE)
            x = x_ref[lines].astype(F32)
            centered = x - jnp.mean(x, axis=-1, keepdims=True)
            variance = jnp.mean(centered * centered, axis=-1, keepdims=True)
            n_ref[lines] = (centered * lax.rsqrt(variance + LN_EPS) * gain).astype(BF16)
        normed = n_ref[span]
        q_ref[span] = (dot(normed, wq_ref[...]) * HEAD_SIZE ** (-0.5)).astype(BF16)
        kv_ref[span] = dot(normed, wkv[...]).astype(BF16)
        pool = dot(normed, wp_ref[...]).astype(BF16)
        p_ref[span] = pool
        part_sum = jnp.sum(pool.astype(F32), axis=0, keepdims=True)
        sums_ref[pl.ds(step * (rows // TILE) + part, 1)] = part_sum
        running = running + part_sum
    total[0:1] = running

    @pl.when(step == last)
    def _():
        hi = running.astype(BF16).astype(F32)
        mid = (running - hi).astype(BF16).astype(F32)
        low = running - hi - mid
        tot = jnp.concatenate([hi, mid, low, jnp.zeros((REACH - 3, pw), F32)], axis=0).astype(BF16)
        tot_ref[...] = tot
        tail_ref[...] = jnp.zeros_like(tail_ref)
        tail_ref[:WINDOW_KEYS, : 2 * kw] = kv_ref[rows - WINDOW_KEYS :]
        tail_ref[WINDOW_KEYS : WINDOW_KEYS + REACH] = p_ref[rows - REACH :]
        tail_ref[WINDOW_KEYS + REACH :] = tot


def project(x, gain, wq, wk, wv, wp):
    length, d = x.shape
    qw, kw, pw = wq.shape[1], wk.shape[1], wp.shape[1]
    rows = min(ROWS, length)
    whole = lambda shape: pl.BlockSpec(shape, lambda i: (0, 0))
    tail_rows = WINDOW_KEYS + 2 * REACH
    return pl.pallas_call(
        project_kernel,
        name="project",
        grid=(length // rows,),
        in_specs=[
            pl.BlockSpec((rows, d), lambda i: (i, 0)),
            whole((1, d)),
            whole((d, qw)),
            whole((d, kw)),
            whole((d, kw)),
            whole((d, pw)),
        ],
        out_specs=[
            pl.BlockSpec((rows, qw), lambda i: (i, 0)),
            pl.BlockSpec((rows, 2 * kw), lambda i: (i, 0)),
            pl.BlockSpec((rows, pw), lambda i: (i, 0)),
            whole((length // TILE, pw)),
            whole((tail_rows, pw)),
            whole((REACH, pw)),
        ],
        out_shape=[
            jax.ShapeDtypeStruct((length, qw), BF16),
            jax.ShapeDtypeStruct((length, 2 * kw), BF16),
            jax.ShapeDtypeStruct((length, pw), BF16),
            jax.ShapeDtypeStruct((length // TILE, pw), F32),
            jax.ShapeDtypeStruct((tail_rows, pw), BF16),
            jax.ShapeDtypeStruct((REACH, pw), BF16),
        ],
        scratch_shapes=[
            pltpu.VMEM((d, 2 * kw), BF16),
            pltpu.VMEM((8, pw), F32),
            pltpu.VMEM((rows, d), BF16),
        ],
        cost_estimate=pl.CostEstimate(
            flops=2 * length * d * (qw + 2 * kw + pw), bytes_accessed=4 * length * d, transcendentals=0
        ),
        compiler_params=pltpu.CompilerParams(dimension_semantics=("arbitrary",)),
    )(x, gain, wq, wk, wv, wp)


def half_of(where, kept):
    return where[0] if kept else 1 - where[0]


def mixer_kernel(further, kept, where_ref, q_ref, kv_ref, kvp_ref, p_ref, pp_ref, sums_ref, tail_ref,
                 *refs):
    tots = refs[:further]
    wg_ref, sink_ref = refs[further : further + 2]
    act_ref, log_ref = refs[-2:]
    seq_part = where_ref[1]
    tile = half_of(where_ref, kept) * pl.num_programs(0) + pl.program_id(0)
    first = tile == 0
    rows, qw = q_ref.shape
    kw = kv_ref.shape[1] // 2
    pw = p_ref.shape[1]
    length = sums_ref.shape[0] * rows

    x = p_ref[...]
    row = lax.broadcasted_iota(jnp.int32, (rows, rows), 0)
    col = lax.broadcasted_iota(jnp.int32, (rows, rows), 1)
    gap = row - col
    lower = jnp.where(gap >= 0, 1.0, 0.0).astype(BF16)
    before = lax.broadcasted_iota(jnp.int32, sums_ref.shape, 0) < tile
    carry = jnp.sum(jnp.where(before, sums_ref[...], 0.0), axis=0, keepdims=True)
    for got in (tail_ref[WINDOW_KEYS + REACH :],) + tuple(t[...] for t in tots):
        carry = carry + jnp.sum(got.astype(F32), axis=0, keepdims=True)
    prev_pool = jnp.where(
        first, tail_ref[WINDOW_KEYS : WINDOW_KEYS + REACH].astype(F32), pp_ref[...].astype(F32)
    ).astype(BF16)
    spot = seq_part * length + tile * rows + lax.broadcasted_iota(jnp.int32, (rows, 1), 0) + 1
    inverse_spot = 1.0 / spot.astype(F32)
    edge_gap = (
        lax.broadcasted_iota(jnp.int32, (REACH, REACH), 0)
        + REACH
        - lax.broadcasted_iota(jnp.int32, (REACH, REACH), 1)
    )
    for slot in range(pw // GDIM):
        lanes = slice(slot * GDIM, (slot + 1) * GDIM)
        width = jnp.left_shift(jnp.int32(2), where_ref[0] * (pw // GDIM) + slot)
        band = jnp.where((gap >= 0) & (gap < width), 1.0, 0.0).astype(BF16)
        edge = jnp.where(edge_gap < width, 1.0, 0.0).astype(BF16)
        window = dot(band, x[:, lanes])
        window = jnp.concatenate(
            [window[:REACH] + dot(edge, prev_pool[:, lanes]), window[REACH:]], axis=0
        )
        prefix = dot(lower, x[:, lanes]) + carry[:, lanes]
        inverse_count = 1.0 / jnp.minimum(spot, width).astype(F32)
        pooled = (window * inverse_count - prefix * inverse_spot).astype(BF16)
        act_ref[:, lanes] = dot(pooled, wg_ref[slot]).astype(BF16)

    wk = WINDOW_KEYS
    key = lax.broadcasted_iota(jnp.int32, (wk, wk), 0)
    query = lax.broadcasted_iota(jnp.int32, (wk, wk), 1)
    is_prev = key > query
    prev_one = jnp.where(is_prev, 1.0, 0.0).astype(BF16)
    own_one = jnp.where(is_prev, 0.0, 1.0).astype(BF16)
    kv_prev = jnp.where(
        first, tail_ref[:wk, : 2 * kw].astype(F32), kvp_ref[...].astype(F32)
    ).astype(BF16)
    no_prev = jnp.where(first & (seq_part == 0), -1e30, 0.0).astype(F32)
    kv_count = kw // HEAD_SIZE
    pairs = qw // HEAD_SIZE // kv_count // 2
    two = 2 * HEAD_SIZE
    for block in range(rows // wk):
        span = slice(block * wk, (block + 1) * wk)
        own = kv_ref[span]
        both = jnp.concatenate([kv_prev, own], axis=0)
        keys = both[:, :kw]
        values_t = both[:, kw:].astype(F32).T.astype(BF16)
        for kv_head in range(kv_count):
            head_key = keys[:, kv_head * HEAD_SIZE : (kv_head + 1) * HEAD_SIZE]
            blank = jnp.zeros_like(head_key)
            stacked = jnp.concatenate(
                [
                    jnp.concatenate([head_key, blank], axis=1),
                    jnp.concatenate([blank, head_key], axis=1),
                ],
                axis=0,
            )
            base = kv_head * pairs
            queries = jnp.concatenate(
                [q_ref[span, (base + p) * two : (base + p + 1) * two] for p in range(pairs)], axis=0
            )
            scores = dot(stacked, queries, ((1,), (1,)))
            head_values = values_t[kv_head * HEAD_SIZE : (kv_head + 1) * HEAD_SIZE]
            halves = []
            for odd in range(2):
                columns = []
                scales = []
                for p in range(pairs):
                    head = (base + p) * 2 + odd
                    cols = slice(p * wk, (p + 1) * wk)
                    seen = jnp.where(
                        is_prev,
                        scores[odd * 2 * wk : odd * 2 * wk + wk, cols] + no_prev
                        if block == 0
                        else scores[odd * 2 * wk : odd * 2 * wk + wk, cols],
                        scores[odd * 2 * wk + wk : (odd + 1) * 2 * wk, cols],
                    )
                    sink = sink_ref[head]
                    row_max = jnp.maximum(jnp.max(seen, axis=0, keepdims=True), sink)
                    weights = jnp.exp(seen - row_max)
                    weight_sum = jnp.sum(weights, axis=0, keepdims=True) + jnp.exp(sink - row_max)
                    log_ref[head : head + 1, span] = row_max + jnp.log(weight_sum)
                    weights = weights.astype(BF16)
                    columns.append(
                        jnp.concatenate([weights * prev_one, weights * own_one], axis=0)
                    )
                    scales.append(1.0 / weight_sum)
                out = dot(head_values, jnp.concatenate(columns, axis=1))
                halves.append(out * jnp.concatenate(scales, axis=1))
            for p in range(pairs):
                cols = slice(p * wk, (p + 1) * wk)
                pair = jnp.concatenate([halves[0][:, cols], halves[1][:, cols]], axis=0).T
                first_lane = pw + (base + p) * two
                act_ref[span, first_lane : first_lane + two] = pair.astype(BF16)
        kv_prev = own


def mix(where, q, kv, pool, sums, tail, tots, w_group, sinks, logs, steps):
    length, qw = q.shape
    kw2, pw = kv.shape[1], pool.shape[1]
    kept = logs is not None
    tile = lambda i, w: half_of(w, kept) * steps + i
    spec = pl.BlockSpec
    heads = qw // HEAD_SIZE
    in_specs = [
        spec((TILE, qw), lambda i, w: (tile(i, w), 0)),
        spec((TILE, kw2), lambda i, w: (tile(i, w), 0)),
        spec((WINDOW_KEYS, kw2), lambda i, w: (jnp.maximum(tile(i, w) * (TILE // WINDOW_KEYS) - 1, 0), 0)),
        spec((TILE, pw), lambda i, w: (tile(i, w), 0)),
        spec((REACH, pw), lambda i, w: (jnp.maximum(tile(i, w) * (TILE // REACH) - 1, 0), 0)),
        spec(sums.shape, lambda i, w: (0, 0)),
        spec(tail.shape, lambda i, w: (0, 0)),
    ]
    in_specs += [spec(t.shape, lambda i, w: (0, 0)) for t in tots]
    in_specs += [
        spec(w_group.shape, lambda i, w: (0, 0, 0)),
        spec(memory_space=pltpu.SMEM),
    ]
    in_specs += [spec(memory_space=pl.ANY)] * kept
    operands = (where, q, kv, kv, pool, pool, sums, tail, *tots, w_group, sinks)
    operands += (logs,) if kept else ()
    return pl.pallas_call(
        lambda *refs: mixer_kernel(len(tots), kept, *refs),
        name="mixer",
        grid_spec=pltpu.PrefetchScalarGridSpec(
            num_scalar_prefetch=1,
            grid=(steps,),
            in_specs=in_specs,
            out_specs=[
                spec((TILE, pw + qw), lambda i, w: (i, 0)),
                spec((heads, TILE), lambda i, w: (0, tile(i, w))),
            ],
        ),
        out_shape=[
            jax.ShapeDtypeStruct((steps * TILE, pw + qw), BF16),
            jax.ShapeDtypeStruct((heads, length), F32),
        ],
        input_output_aliases={len(operands) - 1: 1} if kept else {},
        cost_estimate=pl.CostEstimate(
            flops=8 * steps * TILE * (WINDOW_KEYS * qw + TILE * pw),
            bytes_accessed=6 * steps * TILE * (pw + qw),
            transcendentals=0,
        ),
        compiler_params=pltpu.CompilerParams(dimension_semantics=("arbitrary",)),
    )(*operands)


def output_kernel(where_ref, a_ref, b_ref, wa0, wa1, wb0, wb1, o_ref):
    half = wa0.shape[1]
    total = dot(a_ref[:, :half], wa0[0]) + dot(a_ref[:, half:], wa1[0])
    total = total + dot(b_ref[:, :half], wb0[0]) + dot(b_ref[:, half:], wb1[0])
    o_ref[...] = total.astype(BF16)


def project_out(where, own, other, w_out, width):
    rows, inner = own.shape
    d = w_out.shape[1]
    chunk = inner // 2
    blocks = w_out.reshape(w_out.shape[0] // chunk, chunk, d)
    spec = pl.BlockSpec
    weight = lambda place: spec((1, chunk, width), lambda j, w: (place(w[0]), 0, j))
    return pl.pallas_call(
        output_kernel,
        name="output",
        grid_spec=pltpu.PrefetchScalarGridSpec(
            num_scalar_prefetch=1,
            grid=(d // width,),
            in_specs=[
                spec((rows, inner), lambda j, w: (0, 0)),
                spec((rows, inner), lambda j, w: (0, 0)),
                weight(lambda t: t),
                weight(lambda t: 2 + t),
                weight(lambda t: 1 - t),
                weight(lambda t: 3 - t),
            ],
            out_specs=spec((rows, width), lambda j, w: (0, j)),
        ),
        out_shape=jax.ShapeDtypeStruct((rows, d), BF16),
        cost_estimate=pl.CostEstimate(
            flops=4 * rows * inner * d, bytes_accessed=6 * rows * d, transcendentals=0
        ),
        compiler_params=pltpu.CompilerParams(dimension_semantics=("arbitrary",)),
    )(where, own, other, blocks, blocks, blocks, blocks)


def body(tokens, norm_gain, w_query, w_key, w_value, w_pool, w_group, w_out, sinks):
    x = tokens[0]
    length = x.shape[0]
    parts = lax.axis_size("sp")
    sp, tp = lax.axis_index("sp"), lax.axis_index("tp")
    q, kv, pool, sums, tail, tot = project(
        x, norm_gain[None, :], w_query, w_key, w_value, w_pool
    )
    ahead = lambda value, steps: lax.ppermute(
        value, "sp", [(source, source + steps) for source in range(parts - steps)]
    )
    tail = ahead(tail, 1)
    tots = [ahead(tot, steps) for steps in range(2, parts)]
    steps = length // TILE // 2
    where = jnp.stack([tp, sp]).astype(jnp.int32)
    shared = (where, q, kv, pool, sums, tail, tots, w_group, sinks)
    sent, logs = mix(*shared, None, steps)
    other = lax.ppermute(sent, "tp", [(0, 1), (1, 0)])
    own, logs = mix(*shared, logs, steps)
    mixed = project_out(where, own, other, w_out, 512)
    return (mixed[None], logs[None])


def solution(mesh):
    return jax.shard_map(
        body,
        mesh=mesh,
        in_specs=(
            P("fs", "sp", None),
            P(),
            P(None, "tp"),
            P(None, "tp"),
            P(None, "tp"),
            P(None, "tp"),
            P("tp", None, None),
            P(),
            P("tp"),
        ),
        out_specs=(P("fs", ("sp", "tp"), None), P("fs", "tp", "sp")),
        check_vma=False,
    )
```
